32 devices in a mesh: fs: 8 (over z, y), tp: 4 (over x, core).
Axes of the slice: x: 2, y: 2, z: 4, core: 2. Of those that a mesh axis runs over, the one named last changes fastest.
Arguments:
- inputs: bfloat16 [4096, 3072], P('fs', 'tp'), may hold values from -6 to 6
- cotangent: bfloat16 [4096, 3072], P('fs', 'tp'), may hold values from -6 to 6
- pre_norm: bfloat16 [4096, 3072], P('fs', 'tp'), may hold values from -28 to 28, as said below
- gate_pre: bfloat16 [4096, 5632], P('fs', 'tp'), may hold values from -8 to 8
- value_pre: bfloat16 [4096, 5632], P('fs', 'tp'), may hold values from -6 to 6
- gate_weight: bfloat16 [3072, 5632], P('fs', 'tp'), may hold values from -0.109375 to 0.109375
- value_weight: bfloat16 [3072, 5632], P('fs', 'tp'), may hold values from -0.109375 to 0.109375
- down_weight: bfloat16 [5632, 3072], P('tp', 'fs'), may hold values from -0.078125 to 0.078125
- conv_taps: float32 [3, 5632], P(None, 'tp'), may hold values from -3.5 to 3.5
- norm_gain: float32 [3072], P('tp'), may hold values from 0.1 to 1.9
Outputs:
- grad_input: bfloat16 [4096, 3072], P('fs', 'tp')
- grad_gate: float32 [3072, 5632], P('fs', 'tp')
- grad_value: float32 [3072, 5632], P('fs', 'tp')
- grad_down: float32 [5632, 3072], P('tp', 'fs')
- grad_taps: float32 [3, 5632], P(None, 'tp')
- grad_gain: float32 [3072], P('tp')
The draws below stay inside these ranges and needn't reach their ends.
Inputs may be any that keep to these rules, and one draw needn't show every extreme that they name: `pre_norm`: every entry has magnitude 0.075 or more.
All inputs are finite; a program needn't handle non-finite values.
Results may differ from the reference program's by a relative error of at most 0.014.
Values may be sent and summed in bfloat16 or wider, within the bound.
A program may use at most 128 MiB of HBM per device.

```python
import jax
import jax.numpy as jnp
from jax import lax

D = 3072
FF = 5632
SEQ = 128
TOKENS = 4096
N_TP = 4


def draw_pre_norm(key, part):
    base = jax.random.fold_in(key, 11)
    first, second, third, fourth = jax.random.split(base, 4)
    blocks = jnp.exp(jax.random.uniform(first, (8,), jnp.float32, jnp.log(0.3), jnp.log(3.0)))
    column_scale = jnp.repeat(blocks, D // 8)
    magnitude = 0.5 + jnp.minimum(jnp.abs(jax.random.normal(second, (TOKENS, D), jnp.float32)), 4.0)
    signs = jnp.where(jax.random.bernoulli(third, 0.5, (TOKENS, D)), 1.0, -1.0)
    row_scale = jnp.exp(jax.random.uniform(fourth, (TOKENS, 1), jnp.float32, -0.7, 0.7))
    return (signs * magnitude * column_scale[None, :] * row_scale).astype(jnp.bfloat16)


def strengthened(entries, own_key, source, target, parts, factor):
    owner, partner = [(jnp.arange(entries.shape[axis_at]) // (entries.shape[axis_at] // parts)).reshape([-1 if axis == axis_at else 1 for axis in range(entries.ndim)]) for axis_at in (source, target)]
    chosen = jax.random.permutation(own_key, parts)[partner]
    strong = (owner == chosen) | (owner == (partner + parts // 2) % parts)
    return jnp.where(strong, factor * entries, entries)


def block_scale(key, dims, cuts, low, top_value):
    level, own = 1.0, jax.random.fold_in(key, 6)
    for position, parts in cuts:
        draws = jnp.exp(jax.random.uniform(jax.random.fold_in(own, position), (parts,), jnp.float32, low / len(cuts), top_value / len(cuts)))
        level = level * jnp.repeat(draws, dims[position] // parts).reshape([-1 if axis == position else 1 for axis in range(len(dims))])
    return level


def scatter_about(rng, shape, deviation, bound, cuts=(), kind=jnp.bfloat16):
    level = block_scale(rng, shape, cuts, -0.22, 0.18) if cuts else 1.0
    drawn = jax.random.normal(rng, shape, jnp.float32) * deviation * level
    return jnp.minimum(jnp.maximum(drawn, -bound), bound).astype(kind)


def bell_draw_with(key, shape, width, most, cuts, heavy, kind=jnp.bfloat16):
    result = width * jax.random.normal(key, shape, jnp.float32)
    if cuts:
        result = result * block_scale(key, shape, cuts, -0.22, 0.18)
    return jnp.clip(strengthened(result, jax.random.fold_in(key, 3), *heavy), -most, most).astype(kind)


def setup_inputs(seed: int = 0) -> dict:
    key_of = jax.random.split(jax.random.key(seed), 11)
    inputs = scatter_about(key_of[0], (TOKENS, D), 1.0, 6.0, ((0, 8), (1, 4)))
    cotangent = bell_draw_with(key_of[1], (TOKENS, D), 1.0, 6.0, ((0, 8), (1, 4)), (0, 1, 8, 2.0))
    pre_norm = draw_pre_norm(jax.random.fold_in(key_of[10], 71), 0)
    gate_pre = scatter_about(key_of[3], (TOKENS, FF), 1.5, 8.0, ((0, 8), (1, 4)))
    value_pre = scatter_about(key_of[4], (TOKENS, FF), 1.0, 6.0, ((0, 8), (1, 4)))
    gate_weight = scatter_about(key_of[5], (D, FF), D ** -0.5, 0.109375, ((0, 8), (1, 4)))
    value_weight = scatter_about(key_of[6], (D, FF), D ** -0.5, 0.109375, ((0, 8), (1, 4)))
    down_weight = scatter_about(key_of[7], (FF, D), FF ** -0.5, 0.078125, ((0, 4), (1, 8)))
    conv_taps = scatter_about(key_of[8], (3, FF), 3 ** -0.5, 3.5, ((1, 4),), jnp.float32)
    norm_gain = jnp.clip(1.0 + 0.18 * jax.random.normal(key_of[9], (D,), jnp.float32), 0.1, 1.9)
    return {"inputs": inputs, "cotangent": cotangent, "pre_norm": pre_norm, "gate_pre": gate_pre, "value_pre": value_pre, "gate_weight": gate_weight, "value_weight": value_weight, "down_weight": down_weight, "conv_taps": conv_taps, "norm_gain": norm_gain}


EPSILON = 1e-06

def shifted(values, forward):
    positions = jnp.arange(values.shape[0]) % SEQ
    zeros_row = jnp.zeros((1, values.shape[1]), values.dtype)
    if forward:
        moved = jnp.concatenate([zeros_row, values[:-1]], axis=0)
        keep = positions != 0
    else:
        moved = jnp.concatenate([values[1:], zeros_row], axis=0)
        keep = positions != SEQ - 1
    return jnp.where(keep[:, None], moved, jnp.zeros_like(moved))

def contract_rows(left, right):
    return lax.dot_general(left, right, (((0,), (0,)), ((), ())), preferred_element_type=jnp.float32)

def reference(inputs, cotangent, pre_norm, gate_pre, value_pre, gate_weight, value_weight, down_weight, conv_taps, norm_gain):
    normed = pre_norm.astype(jnp.float32)
    cot_float = cotangent.astype(jnp.float32)
    scaled = norm_gain[None, :] * cot_float
    inverse = lax.rsqrt(lax.optimization_barrier(jnp.sum(normed * normed, axis=1)) / D + EPSILON)
    cross = lax.optimization_barrier(jnp.sum(normed * scaled, axis=1)) / D
    grad_pre = (inverse[:, None] * (scaled - normed * (inverse * inverse * cross)[:, None])).astype(jnp.bfloat16)
    grad_gain = lax.optimization_barrier(jnp.sum(cot_float * normed * inverse[:, None], axis=0))
    gate_float = gate_pre.astype(jnp.float32)
    before = shifted(gate_float, True)
    after = shifted(gate_float, False)
    mixed = conv_taps[0][None] * before + conv_taps[1][None] * gate_float + conv_taps[2][None] * after
    sig = jax.nn.sigmoid(mixed)
    active = mixed * sig
    value_float = value_pre.astype(jnp.float32)
    hidden = (active * value_float).astype(jnp.bfloat16)
    grad_act = lax.dot_general(grad_pre, down_weight, (((1,), (1,)), ((), ())), preferred_element_type=jnp.float32)
    grad_val = (grad_act * active).astype(jnp.bfloat16)
    grad_mixed = grad_act * value_float * sig * (1.0 + mixed * (1.0 - sig))
    grad_taps = jnp.stack([lax.optimization_barrier(jnp.sum(grad_mixed * before, axis=0)), lax.optimization_barrier(jnp.sum(grad_mixed * gate_float, axis=0)), lax.optimization_barrier(jnp.sum(grad_mixed * after, axis=0))], axis=0)
    grad_gpre = (conv_taps[1][None] * grad_mixed + conv_taps[0][None] * shifted(grad_mixed, False) + conv_taps[2][None] * shifted(grad_mixed, True)).astype(jnp.bfloat16)
    block_size = FF // N_TP
    accum = jnp.zeros((inputs.shape[0], D), jnp.float32)
    for block in range(N_TP):
        lower = block * block_size
        upper = lower + block_size
        partial_sum = lax.dot_general(grad_gpre[:, lower:upper], gate_weight[:, lower:upper], (((1,), (1,)), ((), ())), preferred_element_type=jnp.float32)
        partial_sum = partial_sum + lax.dot_general(grad_val[:, lower:upper], value_weight[:, lower:upper], (((1,), (1,)), ((), ())), preferred_element_type=jnp.float32)
        rounded = lax.optimization_barrier(partial_sum.astype(jnp.bfloat16))
        accum = accum + rounded.astype(jnp.float32)
    grad_input = accum.astype(jnp.bfloat16)
    grad_gate = contract_rows(inputs, grad_gpre)
    grad_value = contract_rows(inputs, grad_val)
    grad_down = contract_rows(hidden, grad_pre)
    return (grad_input, grad_gate, grad_value, grad_down, grad_taps, grad_gain)
```

```python
import functools

import jax
import jax.numpy as jnp
from jax import lax
from jax.sharding import PartitionSpec as P


D = 3072
SEQ = 128


EPSILON = 1e-06


def shifted(values, forward):
    positions = jnp.arange(values.shape[0]) % SEQ
    zeros_row = jnp.zeros((1, values.shape[1]), values.dtype)
    if forward:
        moved = jnp.concatenate([zeros_row, values[:-1]], axis=0)
        keep = positions != 0
    else:
        moved = jnp.concatenate([values[1:], zeros_row], axis=0)
        keep = positions != SEQ - 1
    return jnp.where(keep[:, None], moved, jnp.zeros_like(moved))


def contract_rows(left, right):
    return lax.dot_general(
        left, right, (((0,), (0,)), ((), ())), preferred_element_type=jnp.float32
    )


def contract_cols(left, right):
    return lax.dot_general(
        left, right, (((1,), (1,)), ((), ())), preferred_element_type=jnp.float32
    )


def grid_ring(size):
    inner = 1
    while inner * inner * 4 <= size and size % (inner * 2) == 0:
        inner *= 2
    outer = size // inner
    if inner == 1 or outer % 2:
        return list(range(size))
    path = []
    for row in range(outer):
        columns = list(range(1, inner))
        path += [row * inner + column for column in (columns if row % 2 == 0 else columns[::-1])]
    return path + [row * inner for row in reversed(range(outer))]


def ring_gather(block, axis, size):
    order = grid_ring(size)
    ahead = [(order[i], order[(i + 1) % size]) for i in range(size)]
    behind = [(order[(i + 1) % size], order[i]) for i in range(size)]
    rank_of = [0] * size
    for rank, owner in enumerate(order):
        rank_of[owner] = rank
    owners = jnp.array(order, jnp.int32)
    rank = jnp.array(rank_of, jnp.int32)[lax.axis_index(axis)]
    rows = block.shape[0]
    full = jnp.zeros((rows * size, block.shape[1]), block.dtype)

    def placed(full, part, distance, offset):
        owner = owners[lax.rem(rank + distance + size, size)]
        return lax.dynamic_update_slice(full, part, (owner * rows + offset, 0))

    full = placed(full, block, 0, 0)
    forward = backward = block
    for step in range(1, (size - 1) // 2 + 1):
        forward = lax.ppermute(forward, axis, ahead)
        backward = lax.ppermute(backward, axis, behind)
        full = placed(full, forward, -step, 0)
        full = placed(full, backward, step, 0)
    if size % 2 == 0:
        half = rows // 2
        step = size // 2
        upper = lax.ppermute(forward[:half], axis, ahead)
        lower = lax.ppermute(backward[half:], axis, behind)
        full = placed(full, upper, -step, 0)
        full = placed(full, lower, step, half)
    return full


def shift_gather(block, axis, size):
    me = lax.axis_index(axis)
    columns = block.shape[1]
    full = jnp.zeros((block.shape[0], columns * size), block.dtype)
    full = lax.dynamic_update_slice(full, block, (0, me * columns))
    for shift in range(1, size):
        part = lax.ppermute(block, axis, [(i, (i + shift) % size) for i in range(size)])
        owner = lax.rem(me + size - shift, size)
        full = lax.dynamic_update_slice(full, part, (0, owner * columns))
    return full


def shift_scatter(total, axis, size):
    me = lax.axis_index(axis)
    columns = total.shape[1] // size
    result = lax.dynamic_slice(total, (0, me * columns), (total.shape[0], columns)).astype(
        jnp.float32
    )
    for shift in range(1, size):
        target = lax.rem(me + shift, size)
        part = lax.dynamic_slice(total, (0, target * columns), (total.shape[0], columns))
        part = lax.ppermute(part, axis, [(i, (i + shift) % size) for i in range(size)])
        result = result + part.astype(jnp.float32)
    return result.astype(total.dtype)


def on_device(
    n_fs,
    n_tp,
    inputs,
    cotangent,
    pre_norm,
    gate_pre,
    value_pre,
    gate_weight,
    value_weight,
    down_weight,
    conv_taps,
    norm_gain,
):
    normed = pre_norm.astype(jnp.float32)
    cot_float = cotangent.astype(jnp.float32)
    scaled = norm_gain[None, :] * cot_float
    squares, products = lax.psum(
        (jnp.sum(normed * normed, axis=1), jnp.sum(normed * scaled, axis=1)), "tp"
    )
    inverse = lax.rsqrt(squares / D + EPSILON)
    cross = products / D
    grad_pre = (inverse[:, None] * (scaled - normed * (inverse * inverse * cross)[:, None])).astype(
        jnp.bfloat16
    )
    gain_local = jnp.sum(cot_float * normed * inverse[:, None], axis=0)
    grad_full = shift_gather(grad_pre, "tp", n_tp)
    inputs_full = shift_gather(inputs, "tp", n_tp)
    grad_act = contract_cols(grad_full, lax.all_gather(down_weight, "fs", axis=1, tiled=True))
    gate_float = gate_pre.astype(jnp.float32)
    before = shifted(gate_float, True)
    after = shifted(gate_float, False)
    mixed = (
        conv_taps[0][None] * before + conv_taps[1][None] * gate_float + conv_taps[2][None] * after
    )
    sig = jax.nn.sigmoid(mixed)
    active = mixed * sig
    value_float = value_pre.astype(jnp.float32)
    hidden = (active * value_float).astype(jnp.bfloat16)
    grad_val = (grad_act * active).astype(jnp.bfloat16)
    grad_mixed = grad_act * value_float * sig * (1.0 + mixed * (1.0 - sig))
    taps_local = jnp.stack(
        [
            jnp.sum(grad_mixed * before, axis=0),
            jnp.sum(grad_mixed * gate_float, axis=0),
            jnp.sum(grad_mixed * after, axis=0),
        ],
        axis=0,
    )
    grad_gpre = (
        conv_taps[1][None] * grad_mixed
        + conv_taps[0][None] * shifted(grad_mixed, False)
        + conv_taps[2][None] * shifted(grad_mixed, True)
    ).astype(jnp.bfloat16)
    scatter = functools.partial(lax.psum_scatter, axis_name="fs", scatter_dimension=0, tiled=True)
    term_down = contract_rows(grad_full, hidden).astype(jnp.bfloat16)
    term_value = contract_rows(inputs_full, grad_val).astype(jnp.bfloat16)
    term_gate = contract_rows(inputs_full, grad_gpre).astype(jnp.bfloat16)
    grad_down = scatter(term_down).astype(jnp.float32).T
    grad_value = scatter(term_value).astype(jnp.float32)
    grad_gate = scatter(term_gate).astype(jnp.float32)
    value_rows = ring_gather(value_weight, "fs", n_fs)
    late_gate, _ = lax.optimization_barrier((gate_weight, grad_act[:8, :128]))
    gate_rows = ring_gather(late_gate, "fs", n_fs)
    contrib = contract_cols(grad_gpre, gate_rows) + contract_cols(grad_val, value_rows)
    grad_input = shift_scatter(contrib.astype(jnp.bfloat16), "tp", n_tp)
    grad_taps, grad_gain = lax.psum((taps_local, gain_local), "fs")
    return (grad_input, grad_gate, grad_value, grad_down, grad_taps, grad_gain)


def on_device_pairs(
    n_fs,
    n_tp,
    inputs,
    cotangent,
    pre_norm,
    gate_pre,
    value_pre,
    gate_weight,
    value_weight,
    down_weight,
    conv_taps,
    norm_gain,
):
    n_z = n_fs // 2
    me = lax.axis_index("fs")
    upper = me % 2 == 1
    side, level = me % 2, me // 2
    rank = lax.axis_index("tp")

    def swap(value):
        return lax.ppermute(value, "fs", [(i, i ^ 1) for i in range(n_fs)])

    def cross(value, bit):
        return lax.ppermute(value, "tp", [(i, i ^ bit) for i in range(n_tp)])

    def hop(value, sources, step):
        pairs = [(z, z + step) for z in sources]
        return lax.ppermute(value, "fs", [(2 * a + s, 2 * b + s) for a, b in pairs for s in (0, 1)])

    def in_order(own, other, dim):
        return jnp.concatenate(
            [jnp.where(upper, other, own), jnp.where(upper, own, other)], axis=dim
        )

    def stacked(own, other):
        rows = own.shape[0]
        both = jnp.zeros((2 * rows, own.shape[1]), own.dtype)
        both = lax.dynamic_update_slice(both, own, (side * rows, 0))
        return lax.dynamic_update_slice(both, other, ((1 - side) * rows, 0))

    def row_halves(value):
        rows = value.shape[0] // 2
        mine = lax.dynamic_slice_in_dim(value, side * rows, rows, 0)
        return mine, lax.dynamic_slice_in_dim(value, (1 - side) * rows, rows, 0)

    def column_halves(value):
        columns = value.shape[1] // 2
        low, high = value[:, :columns], value[:, columns:]
        return jnp.where(upper, high, low), jnp.where(upper, low, high)

    def blocks_at(value, step):
        columns = value.shape[1] // n_z
        start = lax.rem(level + step, n_z) * columns
        return lax.dynamic_slice(value, (0, start), (value.shape[0], columns))

    class Gather:
        def __init__(self, block):
            self.block, self.up, self.down = block, [block], [block]

        def sends(self):
            step = len(self.up)
            return (
                (self.up[-1], list(range(step - 1, n_z - 1))),
                (self.down[-1], list(range(1, n_z - step + 1))),
            )

        def take(self, up, down):
            self.up.append(up)
            self.down.append(down)

        def full(self):
            rows, columns = self.block.shape
            whole = jnp.zeros((rows, columns * n_z), self.block.dtype)
            for step in range(n_z):
                part = self.block
                if step:
                    part = jnp.where(level + step < n_z, self.down[step], self.up[n_z - step])
                start = lax.rem(level + step, n_z) * columns
                whole = lax.dynamic_update_slice(whole, part, (0, start))
            return whole

    def added(one, other):
        return (one.astype(jnp.float32) + other.astype(jnp.float32)).astype(one.dtype)

    class Reduce:
        def __init__(self, partial):
            self.partial, self.up, self.down, self.step = partial, None, None, 1

        def sends(self):
            rising = blocks_at(self.partial, n_z - self.step)
            falling = blocks_at(self.partial, self.step)
            if self.up is not None:
                rising = added(rising, self.up)
                falling = added(falling, self.down)
            return (
                (rising, list(range(self.step))),
                (falling, list(range(n_z - self.step, n_z))),
            )

        def take(self, up, down):
            self.step += 1
            self.up, self.down = up, down

        def total(self):
            own = blocks_at(self.partial, 0).astype(jnp.float32)
            return own + self.up.astype(jnp.float32) + self.down.astype(jnp.float32)

    def run_round(*lines):
        sends = [line.sends() for line in lines]
        values = []
        sources = []
        here = lax.optimization_barrier(level)
        for way in (0, 1):
            value, levels = sends[0][way]
            for other, more in (send[way] for send in sends[1:]):
                first = here < min(more) if min(more) > max(levels) else here > max(more)
                value = jnp.where(first, value, other)
                levels = levels + more
            values.append(value)
            sources.append(levels)
        up = hop(values[0], sources[0], 1)
        down = hop(values[1], sources[1], -1)
        for line in lines:
            line.take(up, down)

    def gather_cross(block):
        rows, columns = block.shape
        far = cross(block, 2)
        near = cross(block, 1)
        last = cross(far, 1)
        full = jnp.zeros((rows, columns * n_tp), block.dtype)
        for part, bits in ((block, 0), (near, 1), (far, 2), (last, 3)):
            full = lax.dynamic_update_slice(full, part, (0, (rank ^ bits) * columns))
        return full

    mine_down, other_down = row_halves(down_weight)
    down_block = in_order(mine_down, swap(other_down), 1)
    down_block, inputs, gate_pre, value_pre, gate_weight, value_weight = lax.optimization_barrier(
        (down_block, inputs, gate_pre, value_pre, gate_weight, value_weight)
    )
    down_line = Gather(down_block)
    run_round(down_line)

    normed = pre_norm.astype(jnp.float32)
    cot_float = cotangent.astype(jnp.float32)
    scaled = norm_gain[None, :] * cot_float
    sums = jnp.stack([jnp.sum(normed * normed, axis=1), jnp.sum(normed * scaled, axis=1)])
    squares, products = lax.psum(sums, "tp")
    inverse = lax.rsqrt(squares / D + EPSILON)
    cross_term = products / D
    grad_pre = (
        inverse[:, None] * (scaled - normed * (inverse * inverse * cross_term)[:, None])
    ).astype(jnp.bfloat16)
    gain_local = jnp.sum(cot_float * normed * inverse[:, None], axis=0)

    grad_tokens = in_order(grad_pre, swap(grad_pre), 0)
    gate_mine, gate_other = column_halves(gate_pre)
    value_mine, value_other = column_halves(value_pre)
    gate_tokens = in_order(gate_mine, swap(gate_other), 0)
    value_tokens = in_order(value_mine, swap(value_other), 0)
    grad_full = gather_cross(grad_tokens)
    run_round(down_line)

    taps = row_halves(conv_taps.T)[0].T
    gate_float = gate_tokens.astype(jnp.float32)
    before = shifted(gate_float, True)
    after = shifted(gate_float, False)
    mixed = taps[0][None] * before + taps[1][None] * gate_float + taps[2][None] * after
    sig = jax.nn.sigmoid(mixed)
    active = mixed * sig
    value_float = value_tokens.astype(jnp.float32)
    hidden = (active * value_float).astype(jnp.bfloat16)
    down_sum = Reduce(contract_rows(hidden, grad_full).astype(jnp.bfloat16))

    def weight_block(weight):
        mine, other = row_halves(weight.T)
        return in_order(mine, swap(other), 1)

    value_line = Gather(weight_block(value_weight))
    run_round(value_line)
    run_round(down_line, down_sum)

    input_tokens = stacked(inputs, swap(inputs))
    inputs_full = gather_cross(input_tokens)

    gate_line = Gather(weight_block(gate_weight))
    run_round(gate_line)

    grad_act = contract_cols(grad_full, down_line.full())
    grad_val = (grad_act * active).astype(jnp.bfloat16)
    grad_mixed = grad_act * value_float * sig * (1.0 + mixed * (1.0 - sig))
    taps_local = jnp.stack(
        [
            jnp.sum(grad_mixed * before, axis=0),
            jnp.sum(grad_mixed * gate_float, axis=0),
            jnp.sum(grad_mixed * after, axis=0),
        ],
        axis=0,
    )
    grad_gpre = (
        taps[1][None] * grad_mixed
        + taps[0][None] * shifted(grad_mixed, False)
        + taps[2][None] * shifted(grad_mixed, True)
    ).astype(jnp.bfloat16)
    value_sum = Reduce(contract_rows(grad_val, inputs_full).astype(jnp.bfloat16))
    gate_sum = Reduce(contract_rows(grad_gpre, inputs_full).astype(jnp.bfloat16))
    run_round(value_line, value_sum)
    run_round(gate_line, gate_sum)
    run_round(value_line, down_sum)
    run_round(gate_line, value_sum)
    run_round(gate_sum)
    run_round(down_sum)
    run_round(value_sum)
    run_round(gate_sum)
    value_full, gate_full = value_line.full(), gate_line.full()

    def token_half(which):
        rows = grad_val.shape[0] // 2
        val = lax.dynamic_slice_in_dim(grad_val, which * rows, rows, 0)
        pre = lax.dynamic_slice_in_dim(grad_gpre, which * rows, rows, 0)
        dims = (((1,), (0,)), ((), ()))
        total = lax.dot_general(val, value_full, dims, preferred_element_type=jnp.float32)
        total = total + lax.dot_general(pre, gate_full, dims, preferred_element_type=jnp.float32)
        total = total.astype(jnp.bfloat16)
        columns = total.shape[1] // n_tp

        def owned(bits):
            return lax.dynamic_slice(total, (0, (rank ^ bits) * columns), (rows, columns))

        arrived = cross(jnp.concatenate([owned(1), owned(3)], axis=1), 1).astype(jnp.float32)
        far = owned(2).astype(jnp.float32) + arrived[:, columns:]
        near = owned(0).astype(jnp.float32) + arrived[:, :columns]
        return near + cross(far.astype(jnp.bfloat16), 2).astype(jnp.float32)

    theirs = token_half(1 - side)
    ours = token_half(side)
    grad_input = (ours + swap(theirs.astype(jnp.bfloat16)).astype(jnp.float32)).astype(jnp.bfloat16)

    def placed(total):
        mine, other = total[:, : total.shape[1] // 2], total[:, total.shape[1] // 2 :]
        keep = jnp.where(upper, other, mine)
        send = jnp.where(upper, mine, other).astype(jnp.bfloat16)
        return in_order(keep, swap(send).astype(jnp.float32), 0)

    grad_down = placed(down_sum.total())
    grad_value = placed(value_sum.total()).T
    grad_gate = placed(gate_sum.total()).T

    empty = jnp.zeros_like(taps_local)
    spread = jnp.concatenate(
        [jnp.where(upper, empty, taps_local), jnp.where(upper, taps_local, empty)], axis=1
    )
    small = jnp.concatenate([spread.reshape(-1), gain_local])

    def sent(value, mask):
        return lax.ppermute(value, "fs", [(i, i ^ mask) for i in range(n_fs)])

    small = small + sent(small, 1)
    small = (small + sent(small, 2)) + (sent(small, 4) + sent(small, 6))
    grad_taps = small[: spread.size].reshape(spread.shape)
    grad_gain = small[spread.size :]
    return (grad_input, grad_gate, grad_value, grad_down, grad_taps, grad_gain)


def in_one_layer(*args):
    return on_device_pairs(*args)


def pairs_fit(n_fs, n_tp):
    return n_tp == 4 and n_fs == 2 * n_tp


def solution(mesh):
    in_specs = (
        P("fs", "tp"),
        P("fs", "tp"),
        P("fs", "tp"),
        P("fs", "tp"),
        P("fs", "tp"),
        P("fs", "tp"),
        P("fs", "tp"),
        P("tp", "fs"),
        P(None, "tp"),
        P("tp"),
    )
    out_specs = (P("fs", "tp"), P("fs", "tp"), P("fs", "tp"), P("tp", "fs"), P(None, "tp"), P("tp"))
    n_fs, n_tp = mesh.shape["fs"], mesh.shape["tp"]
    paired = pairs_fit(n_fs, n_tp)
    body = in_one_layer if paired else on_device
    return jax.shard_map(
        functools.partial(body, n_fs, n_tp),
        mesh=mesh,
        in_specs=in_specs,
        out_specs=out_specs,
        check_vma=False,
    )
```
